32 devices in a mesh: fs: 8 (over z, y), tp: 4 (over x, core).
Axes of the slice: x: 2, y: 2, z: 4, core: 2. Of those that a mesh axis runs over, the one named last changes fastest.
Arguments:
- tokens: bfloat16 [3072, 2048], P('fs', 'tp'), may hold values from -6 to 6
- norm_gain: float32 [2048], P('fs'), may hold values from 0.1 to 1.9
- gate_train: bfloat16 [8, 2048, 5632], P(None, 'fs', 'tp'), may hold values from -0.125 to 0.125
- up_train: bfloat16 [8, 2048, 5632], P(None, 'fs', 'tp'), may hold values from -0.125 to 0.125
- down_train: bfloat16 [8, 2048, 5632], P(None, 'fs', 'tp'), may hold values from -0.078125 to 0.078125
- routes: int32 [3072, 2], P('fs'), may hold values from 0 to 7, all different within a row; in each aligned block of 384 rows (0 to 383, 384 to 767, ...) at most 192 rows name the same one
- route_logits: float32 [3072, 2], P('fs'), may hold values from -6 to 6
Outputs:
- gate_weights: bfloat16 [8, 2048, 5632], P('fs', None, 'tp')
- up_weights: bfloat16 [8, 2048, 5632], P('fs', None, 'tp')
- down_weights: bfloat16 [8, 2048, 5632], P('fs', None, 'tp')
- mixed: bfloat16 [3072, 2048], P('fs', 'tp')
The draws below stay inside these ranges and needn't reach their ends.
Inputs may be any that keep to these rules, and one draw needn't show every extreme that they name: `routes`: each row names 2 different experts; among the rows of one device no expert is named more than 192 times, and in every draw some device names some expert exactly 192 times.
All inputs are finite; a program needn't handle non-finite values.
Results may differ from the reference program's by a relative error of at most 0.014.
Values may be sent and summed in bfloat16 or wider, within the bound.
A program may use at most 128 MiB of HBM per device.

```python
import math
import jax
import jax.numpy as jnp
import numpy as np
from jax import lax

D = 2048
FF = 5632
EXPERTS = 8
TOP = 2
TOK_DEV = 384
TOKENS = 3072
MOST = 192
N_FS = 8
N_TP = 4


def levels(stream_key, shape, cuts, least, high):
    loudness = 1.0
    for axis_at, parts in cuts:
        heights = jax.random.uniform(jax.random.fold_in(jax.random.fold_in(stream_key, 6), axis_at), (parts,), jnp.float32, least / len(cuts), high / len(cuts))
        loudness = loudness * jnp.repeat(jnp.exp(heights), shape[axis_at] // parts).reshape((-1,) + (1,) * (len(shape) - 1 - axis_at))
    return loudness


def shared_out(stream_key, own, number, rows, amount, top, reach, lean):
    ranking = jax.random.permutation(stream_key, amount)
    crowded, ordinary = load_shares(amount, rows * top, reach, lean, True), load_shares(amount, rows * top, reach, lean, False)
    places = jnp.arange(amount)

    def named(tallies, offset_by):
        used = int((tallies > 0).sum())
        fixed = max(1, used // 4)
        moved = fixed + (places - fixed + offset_by * (used - fixed)) % max(1, amount - fixed)
        return jnp.zeros((amount,), jnp.int32).at[ranking[jnp.where(places < fixed, places, moved)]].set(jnp.asarray(tallies, jnp.int32))

    tallies = jnp.where(number % 4 == 0, named(crowded, number // 4), named(ordinary, number - number // 4 - 1))
    mixed = jax.random.permutation(jax.random.fold_in(own, 3), amount)
    giver, taker = mixed[0:amount // 2 * 2:2], mixed[1:amount // 2 * 2:2]
    slack = jnp.minimum(tallies[giver] - 1, reach - tallies[taker]) // 2
    slack = jnp.where((giver == ranking[0]) | (taker == ranking[0]) | (tallies[taker] == 0), 0, jnp.maximum(slack, 0))
    moved = jax.random.randint(jax.random.fold_in(own, 4), (amount // 2,), 0, 1 << 20) % (slack + 1)
    tallies = tallies.at[giver].add(-moved).at[taker].add(moved)
    labels = jnp.searchsorted(jnp.cumsum(tallies), jnp.arange(rows * top), side="right").astype(jnp.int32)
    table = labels.reshape(top, rows).T
    table = table[jax.random.permutation(jax.random.fold_in(own, 1), rows)]
    offset_by = jax.random.randint(jax.random.fold_in(own, 2), (rows, 1), 0, top)
    return jnp.take_along_axis(table, (jnp.arange(top)[None, :] + offset_by) % top, axis=1)


def load_shares(count, total, bound, slope, full):
    weights = [(1 << 20) // math.isqrt(grade ** slope) + 1 for grade in range(1, count + 1)]
    largest = bound if full else min(bound, max(-(-total // count), total * weights[0] // sum(weights)))
    least = 1 if total - largest >= count - 1 else 0
    given, spare = [largest] + [least] * (count - 1), total - largest - least * (count - 1)
    while spare > 0:
        free = [i for i in range(1, count) if given[i] < largest] or [i for i in range(1, count) if given[i] < bound]
        pool, budget = sum([weights[i] for i in free]), spare
        for i in free:
            more = min(bound - given[i], max(1, budget * weights[i] // pool), spare)
            given[i] = given[i] + more
            spare = spare - more
    return np.array(given)


def scatter_about(key, shape, deviation, limit, cuts=(), held_as=jnp.bfloat16):
    values = deviation * jax.random.normal(key, shape, jnp.float32)
    if cuts:
        values = values * levels(key, shape, cuts, -0.22, 0.18)
    return jnp.clip(values, -limit, limit).astype(held_as)


def setup_inputs(seed: int = 0) -> dict:
    key_list = jax.random.split(jax.random.key(seed), 8)
    tokens = scatter_about(key_list[0], (TOKENS, D), 1.0, 6.0, ((0, 8), (1, 4)))
    norm_gain = jnp.clip(1.0 + 0.18 * jax.random.normal(key_list[1], (D,), jnp.float32), 0.1, 1.9)
    gate_train = scatter_about(key_list[2], (EXPERTS, D, FF), D ** -0.5, 0.125, ((1, 8), (2, 4)))
    up_train = scatter_about(key_list[3], (EXPERTS, D, FF), D ** -0.5, 0.125, ((1, 8), (2, 4)))
    down_train = scatter_about(key_list[4], (EXPERTS, D, FF), FF ** -0.5, 0.078125, ((1, 8), (2, 4)))
    routes_keys = jax.random.split(jax.random.fold_in(key_list[5], 1), TOKENS // TOK_DEV)
    routes_turns = jax.random.permutation(jax.random.fold_in(key_list[5], 3), TOKENS // TOK_DEV)
    routes = jax.vmap(lambda own, number: shared_out(jax.random.fold_in(key_list[5], 2), own, number, TOK_DEV, EXPERTS, TOP, TOK_DEV // 2, 1))(routes_keys, routes_turns).reshape((TOKENS, TOP))
    route_logits = scatter_about(key_list[6], (TOKENS, TOP), 1.5, 6.0, ((0, 8),), jnp.float32)
    return {"tokens": tokens, "norm_gain": norm_gain, "gate_train": gate_train, "up_train": up_train, "down_train": down_train, "routes": routes, "route_logits": route_logits}


def reference(tokens, norm_gain, gate_train, up_train, down_train, routes, route_logits):
    slot_expert = jnp.arange(N_FS, dtype=jnp.int32) % EXPERTS
    gain_rows = norm_gain[None, :, None]
    gate_low = (gate_train.astype(jnp.float32) * gain_rows).astype(jnp.bfloat16)
    up_low = (up_train.astype(jnp.float32) * gain_rows).astype(jnp.bfloat16)
    down_low = down_train.astype(jnp.bfloat16)
    gate_weights = gate_low[slot_expert]
    up_weights = up_low[slot_expert]
    down_weights = down_low[slot_expert]
    tok_float = tokens.astype(jnp.float32)
    inverse = lax.rsqrt(lax.optimization_barrier(jnp.mean(tok_float * tok_float, axis=1, keepdims=True)) + 1e-06)
    normed = (tok_float * inverse).astype(jnp.bfloat16)
    padded = jnp.concatenate([normed, jnp.zeros((1, D), jnp.bfloat16)], axis=0)
    by_device = routes.reshape(N_FS, TOK_DEV * TOP)
    onehot = (by_device[:, :, None] == jnp.arange(EXPERTS, dtype=jnp.int32)[None, None, :]).astype(jnp.int32)
    order_rank = lax.optimization_barrier(jnp.sum((jnp.cumsum(onehot, axis=1) - onehot) * onehot, axis=2))
    position = (jnp.arange(N_FS, dtype=jnp.int32)[:, None] * MOST + order_rank).reshape(-1).astype(jnp.int32)
    flat_routes = by_device.reshape(-1)
    token_of = (jnp.arange(TOKENS * TOP, dtype=jnp.int32) // TOP).astype(jnp.int32)
    width = FF // N_TP
    results = []
    for expert in range(EXPERTS):
        spots = jnp.where(flat_routes == expert, position, N_FS * MOST).astype(jnp.int32)
        table = jnp.full((N_FS * MOST,), TOKENS, jnp.int32).at[spots].set(token_of, mode='drop')
        rows_in = padded[table]
        gate_val = jnp.dot(rows_in, gate_low[expert], preferred_element_type=jnp.float32)
        up_val = jnp.dot(rows_in, up_low[expert], preferred_element_type=jnp.float32)
        active = (jax.nn.silu(gate_val) * up_val).astype(jnp.bfloat16)
        total = jnp.zeros((N_FS * MOST, D), jnp.float32)
        for block in range(N_TP):
            partial_value = lax.dot_general(active[:, block * width:(block + 1) * width], down_low[expert][:, block * width:(block + 1) * width], (((1,), (1,)), ((), ())), preferred_element_type=jnp.float32)
            rounded = lax.optimization_barrier(partial_value.astype(jnp.bfloat16))
            total = total + rounded.astype(jnp.float32)
        results.append(total.astype(jnp.bfloat16))
    stacked = jnp.stack(results, axis=0)
    picked = stacked[flat_routes, position].astype(jnp.float32).reshape(TOKENS, TOP, D)
    first = jax.nn.sigmoid(route_logits[:, 0] - route_logits[:, 1])
    second = jax.nn.sigmoid(route_logits[:, 1] - route_logits[:, 0])
    mixed = (picked[:, 0, :] * first[:, None] + picked[:, 1, :] * second[:, None]).astype(jnp.bfloat16)
    return (gate_weights, up_weights, down_weights, mixed)
```

```python
import functools

import jax
import jax.numpy as jnp
from jax import lax
from jax.experimental import pallas as pl
from jax.experimental.pallas import tpu as pltpu
from jax.sharding import PartitionSpec as P

EXPERTS = 8
EPSILON = 1e-06
MESH = pl.DeviceIdType.MESH
F32 = jnp.float32
BF16 = jnp.bfloat16
NT = (((1,), (1,)), ((), ()))
TN = (((0,), (0,)), ((), ()))


def shift_of(step, n):
    return n // 2 + (1 - 2 * (step % 2)) * ((step + 1) // 2)


def kernel(
    n, m, tokens, gain, gate_hbm, up_hbm, down_hbm, routes, logits,
    gate_out, up_out, down_out, mixed,
    stage, weights, outgoing, rows, active, picks, ranks, scales, mix_high, mix_low,
    parts, landed, result, returned,
    load_sem, w_send, w_recv, d_send, d_recv, f_send, f_recv, p_send, p_recv, r_send, r_recv, o_sem,
):
    me = lax.axis_index("fs")
    tp = lax.axis_index("tp")
    copies = n // EXPERTS
    tok_rows, feats = tokens.shape
    cap = tok_rows // 2 // copies
    slots = n * cap
    depth = weights.shape[1] // n
    per = n // m

    def load(w, e):
        source = (gate_hbm, up_hbm)[w]
        return pltpu.make_async_copy(source.at[e], stage.at[w, e], load_sem.at[w, e])

    for w in range(2):
        for e in range(EXPERTS):
            load(w, e).start()
    mine = weights.at[2, pl.ds(pl.multiple_of(me * depth, depth), depth)]
    own_down = pltpu.make_async_copy(down_hbm.at[me % EXPERTS], mine, load_sem.at[2, 0])
    own_down.start()

    barrier = pltpu.get_barrier_semaphore()

    @pl.loop(1, n)
    def _(k):
        pl.semaphore_signal(
            barrier, inc=1, device_id=((me + k) % n, tp), device_id_type=MESH
        )

    @pl.loop(1, m)
    def _(k):
        pl.semaphore_signal(
            barrier, inc=1, device_id=(me, (tp + k) % m), device_id_type=MESH
        )

    first, second = routes[0:1, :], routes[1:2, :]
    ids = lax.broadcasted_iota(jnp.int32, (EXPERTS, tok_rows), 0)
    named = ((ids == first) | (ids == second)).astype(F32)
    before = lax.broadcasted_iota(jnp.int32, (tok_rows, tok_rows), 0)
    after = lax.broadcasted_iota(jnp.int32, (tok_rows, tok_rows), 1)
    earlier = (before < after).astype(F32).astype(BF16)
    picks[...] = named
    ranks[...] = jnp.dot(named.astype(BF16), earlier, preferred_element_type=F32)
    gap = logits[0:1, :] - logits[1:2, :]
    scales[...] = jnp.where(ids == first, jax.nn.sigmoid(gap), jax.nn.sigmoid(-gap))

    pl.semaphore_wait(barrier, n - 1 + m - 1)

    def dispatch(k):
        target = (me + k) % n
        return pltpu.make_async_remote_copy(
            src_ref=outgoing.at[pl.ds(pl.multiple_of(target * cap, cap), cap)],
            dst_ref=rows.at[
                pl.ds(pl.multiple_of(me * cap, cap), cap),
                pl.ds(pl.multiple_of(tp * feats, feats), feats),
            ],
            send_sem=d_send.at[k],
            recv_sem=d_recv.at[k],
            device_id=(target, tp),
            device_id_type=MESH,
        )

    def fill(target):
        e = target % EXPERTS
        want = (
            lax.broadcasted_iota(jnp.int32, (cap, tok_rows), 0) * copies + target // EXPERTS
        ).astype(F32)
        hit = (ranks[pl.ds(e, 1), :] == want) & (picks[pl.ds(e, 1), :] > 0.5)
        where = pl.ds(pl.multiple_of(target * cap, cap), cap)
        chosen = jnp.where(hit, 1.0, 0.0).astype(BF16)
        moved = jnp.dot(chosen, tokens[...], preferred_element_type=F32).astype(BF16)
        outgoing[where, :] = moved
        scale = jnp.where(hit, scales[pl.ds(e, 1), :], 0.0)
        high = scale.astype(BF16)
        mix_high[where, :] = high
        mix_low[where, :] = (scale - high.astype(F32)).astype(BF16)
        return moved

    @pl.loop(0, n - 1)
    def _(i):
        k = shift_of(i, n)
        fill((me + k) % n)
        dispatch(k).start()

    rows[
        pl.ds(pl.multiple_of(me * cap, cap), cap),
        pl.ds(pl.multiple_of(tp * feats, feats), feats),
    ] = fill(me)

    def give(w, k):
        target = (me + k) % n
        e = target % EXPERTS
        return pltpu.make_async_remote_copy(
            src_ref=down_hbm.at[e] if w == 2 else stage.at[w, e],
            dst_ref=weights.at[w, pl.ds(pl.multiple_of(me * depth, depth), depth)],
            send_sem=w_send.at[w, k],
            recv_sem=w_recv.at[w, k],
            device_id=(target, tp),
            device_id_type=MESH,
        )

    for w in range(2):
        for e in range(EXPERTS):
            load(w, e).wait()

        @pl.loop(0, EXPERTS)
        def _(e):
            stage[w, pl.ds(e, 1)] = (
                stage[w, pl.ds(e, 1)].astype(F32) * gain[...][None]
            ).astype(BF16)

        @pl.loop(0, n - 1)
        def _(i):
            give(w, shift_of(i, n)).start()

        weights[w, pl.ds(pl.multiple_of(me * depth, depth), depth), :] = stage[
            w, pl.ds(me % EXPERTS, 1)
        ][0]

    @pl.loop(0, n - 1)
    def _(i):
        give(2, shift_of(i, n)).start()

    def share(k):
        block = rows.at[:, pl.ds(pl.multiple_of(tp * feats, feats), feats)]
        return pltpu.make_async_remote_copy(
            src_ref=block,
            dst_ref=block,
            send_sem=f_send.at[k],
            recv_sem=f_recv.at[k],
            device_id=(me, (tp + k) % m),
            device_id_type=MESH,
        )

    @pl.loop(1, n)
    def _(k):
        dispatch(k).wait()

    @pl.loop(1, m)
    def _(k):
        share(k).start()

    @pl.loop(1, m)
    def _(k):
        share(k).wait()

    tile = slots // 12

    @pl.loop(0, slots // tile)
    def _(i):
        where = pl.ds(pl.multiple_of(i * tile, tile), tile)
        value = rows[where, :].astype(F32)
        inverse = lax.rsqrt(jnp.mean(value * value, axis=1, keepdims=True) + EPSILON)
        rows[where, :] = (value * inverse).astype(BF16)

    outs = []
    for w in range(2):

        @pl.loop(1, n)
        def _(k):
            give(w, k).wait()

        outs.append(
            pltpu.make_async_copy(weights.at[w], (gate_out, up_out)[w].at[0], o_sem.at[w])
        )
        outs[w].start()

    big = slots // 6

    @pl.loop(0, slots // big)
    def _(i):
        where = pl.ds(pl.multiple_of(i * big, big), big)
        value = rows[where, :]
        gate_val = jnp.dot(value, weights[0], preferred_element_type=F32)
        up_val = jnp.dot(value, weights[1], preferred_element_type=F32)
        active[where, :] = (gate_val / (1.0 + jnp.exp(-gate_val)) * up_val).astype(BF16)

    def source_of(i):
        k = jnp.where(i == 0, 0, shift_of(jnp.maximum(i - 1, 0), n))
        return k, (me + n - k) % n

    def hand(j):
        owner = j // per
        k = (owner + m - tp) % m
        return pltpu.make_async_remote_copy(
            src_ref=parts.at[j],
            dst_ref=landed.at[j % per, k],
            send_sem=p_send.at[j],
            recv_sem=p_recv.at[j % per, k],
            device_id=(me, owner),
            device_id_type=MESH,
        )

    def taken(q, k):
        return pltpu.make_async_remote_copy(
            src_ref=parts.at[0],
            dst_ref=landed.at[q, k],
            send_sem=p_send.at[0],
            recv_sem=p_recv.at[q, k],
            device_id=(me, (tp + k) % m),
            device_id_type=MESH,
        )

    def back(q, k):
        target = (me + k) % n
        return pltpu.make_async_remote_copy(
            src_ref=result.at[q, pl.ds(pl.multiple_of(target * cap, cap), cap)],
            dst_ref=returned.at[q, pl.ds(pl.multiple_of(me * cap, cap), cap)],
            send_sem=r_send.at[q, k],
            recv_sem=r_recv.at[q, k],
            device_id=(target, tp),
            device_id_type=MESH,
        )

    own_down.wait()
    half = slots // 4

    @pl.loop(0, n + 1)
    def _(i):
        @pl.when(i < n)
        def _():
            k, j = source_of(i)

            @pl.when(i > 0)
            def _():
                give(2, k).wait()

            rhs = weights[2, pl.ds(pl.multiple_of(j * depth, depth), depth), :]

            @pl.loop(0, slots // half)
            def _(r):
                where = pl.ds(pl.multiple_of(r * half, half), half)
                parts[j, where, :] = lax.dot_general(
                    active[where, :], rhs, NT, preferred_element_type=F32
                ).astype(BF16)

            @pl.when(j // per != tp)
            def _():
                hand(j).start()

        @pl.when(i > 0)
        def _():
            _, j = source_of(jnp.maximum(i - 1, 0))
            q = j % per

            @pl.when(j // per == tp)
            def _():
                @pl.loop(1, m)
                def _(k):
                    taken(q, k).wait_recv()

                @pl.loop(0, slots // half)
                def _(r):
                    where = pl.ds(pl.multiple_of(r * half, half), half)
                    total = parts[j, where, :].astype(F32)
                    for k in range(1, m):
                        total = total + landed[q, k, where, :].astype(F32)
                    result[q, where, :] = total.astype(BF16)

                @pl.loop(0, n - 1)
                def _(s):
                    back(q, shift_of(s, n)).start()

                mine = pl.ds(pl.multiple_of(me * cap, cap), cap)
                returned[q, mine, :] = result[q, mine, :]

    last = pltpu.make_async_copy(weights.at[2], down_out.at[0], o_sem.at[2])
    last.start()

    @pl.loop(0, n)
    def _(j):
        @pl.when(j // per != tp)
        def _():
            hand(j).wait_send()

    for q in range(per):

        @pl.loop(1, n)
        def _(k):
            back(q, k).wait()

        value = returned[q]
        total = lax.dot_general(mix_high[...], value, TN, preferred_element_type=F32)
        total += lax.dot_general(mix_low[...], value, TN, preferred_element_type=F32)
        mixed[:, q * depth : (q + 1) * depth] = total.astype(BF16)

    for out in outs:
        out.wait()
    last.wait()


def shards(n, m, tokens, norm_gain, gate_train, up_train, down_train, routes, route_logits):
    experts, depth, width = gate_train.shape
    tok_rows, feats = tokens.shape
    copies = n // experts
    cap = tok_rows // 2 // copies
    slots = n * cap
    per = n // m
    full = jax.ShapeDtypeStruct((1, depth * n, width), BF16)
    vmem = pl.BlockSpec(memory_space=pltpu.VMEM)
    hbm = pl.BlockSpec(memory_space=pl.ANY)
    dma = pltpu.SemaphoreType.DMA
    return pl.pallas_call(
        functools.partial(kernel, n, m),
        out_shape=(full, full, full, jax.ShapeDtypeStruct((tok_rows, feats), BF16)),
        in_specs=[vmem, vmem, hbm, hbm, hbm, vmem, vmem],
        out_specs=(hbm, hbm, hbm, vmem),
        scratch_shapes=[
            pltpu.VMEM((2, experts, depth, width), BF16),
            pltpu.VMEM((3, depth * n, width), BF16),
            pltpu.VMEM((slots, feats), BF16),
            pltpu.VMEM((slots, feats * m), BF16),
            pltpu.VMEM((slots, width), BF16),
            pltpu.VMEM((experts, tok_rows), F32),
            pltpu.VMEM((experts, tok_rows), F32),
            pltpu.VMEM((experts, tok_rows), F32),
            pltpu.VMEM((slots, tok_rows), BF16),
            pltpu.VMEM((slots, tok_rows), BF16),
            pltpu.VMEM((n, slots, depth), BF16),
            pltpu.VMEM((per, m, slots, depth), BF16),
            pltpu.VMEM((per, slots, depth), BF16),
            pltpu.VMEM((per, slots, depth), BF16),
            dma((3, experts)),
            dma((3, n)),
            dma((3, n)),
            dma((n,)),
            dma((n,)),
            dma((m,)),
            dma((m,)),
            dma((n,)),
            dma((per, m)),
            dma((per, n)),
            dma((per, n)),
            dma((3,)),
        ],
        compiler_params=pltpu.CompilerParams(
            collective_id=0, has_side_effects=True, vmem_limit_bytes=67043328
        ),
    )(
        tokens,
        norm_gain[:, None],
        gate_train,
        up_train,
        down_train,
        routes.T,
        route_logits.T,
    )


def solution(mesh):
    weight = P(None, "fs", "tp")
    placed = (P("fs", "tp"), P("fs"), weight, weight, weight, P("fs", None), P("fs", None))
    copy = P("fs", None, "tp")
    return jax.shard_map(
        functools.partial(shards, mesh.shape["fs"], mesh.shape["tp"]),
        mesh=mesh,
        in_specs=placed,
        out_specs=(copy, copy, copy, P("fs", "tp")),
        check_vma=False,
    )
```

```python
import functools

import jax
import jax.numpy as jnp
from jax import lax
from jax.experimental import pallas as pl
from jax.experimental.pallas import tpu as pltpu
from jax.sharding import PartitionSpec as P

EXPERTS = 8
EPSILON = 1e-06
MESH = pl.DeviceIdType.MESH
F32 = jnp.float32
BF16 = jnp.bfloat16
NT = (((1,), (1,)), ((), ()))
TN = (((0,), (0,)), ((), ()))


def shift_of(step, n):
    return n // 2 + (1 - 2 * (step % 2)) * ((step + 1) // 2)


def kernel(
    n, m, tokens, gain, gate_hbm, up_hbm, down_hbm, routes, logits,
    gate_out, up_out, down_out, mixed,
    stage, weights, gathered, tables, rows, active, ranks, scales, mix_high, mix_low,
    parts, landed, result, returned,
    load_sem, w_send, w_recv, a_send, a_recv, b_send, b_recv, f_send, f_recv, p_send, p_recv, r_send, r_recv, o_sem,
):
    me = lax.axis_index("fs")
    tp = lax.axis_index("tp")
    copies = n // EXPERTS
    tok_rows, feats = tokens.shape
    cap = tok_rows // 2 // copies
    slots = n * cap
    depth = weights.shape[1] // n
    per = n // m

    def load(w, e):
        source = (gate_hbm, up_hbm)[w]
        return pltpu.make_async_copy(source.at[e], stage.at[w, e], load_sem.at[w, e])

    for w in range(2):
        for e in range(EXPERTS):
            load(w, e).start()
    mine = weights.at[2, pl.ds(pl.multiple_of(me * depth, depth), depth)]
    own_down = pltpu.make_async_copy(down_hbm.at[me % EXPERTS], mine, load_sem.at[2, 0])
    own_down.start()

    barrier = pltpu.get_barrier_semaphore()

    @pl.loop(1, n)
    def _(k):
        pl.semaphore_signal(
            barrier, inc=1, device_id=((me + k) % n, tp), device_id_type=MESH
        )

    @pl.loop(1, m)
    def _(k):
        pl.semaphore_signal(
            barrier, inc=1, device_id=(me, (tp + k) % m), device_id_type=MESH
        )

    first, second = routes[0:1, :], routes[1:2, :]
    ids = lax.broadcasted_iota(jnp.int32, (EXPERTS, tok_rows), 0)
    named = ((ids == first) | (ids == second)).astype(F32)
    before = lax.broadcasted_iota(jnp.int32, (tok_rows, tok_rows), 0)
    after = lax.broadcasted_iota(jnp.int32, (tok_rows, tok_rows), 1)
    earlier = (before < after).astype(F32).astype(BF16)
    rank = jnp.dot(named.astype(BF16), earlier, preferred_element_type=F32)
    ranks[...] = jnp.where(named > 0.5, rank, -1.0)
    gap = logits[0:1, :] - logits[1:2, :]
    scales[...] = jnp.where(ids == first, jax.nn.sigmoid(gap), jax.nn.sigmoid(-gap))

    pl.semaphore_wait(barrier, n - 1 + m - 1)

    side = n // 2
    base = me // side * side
    partner = (me + side) % n

    def spread(w, k):
        target = jnp.where(k == 0, partner, base + (me + k) % side)
        return pltpu.make_async_remote_copy(
            src_ref=(tokens, ranks)[w],
            dst_ref=(gathered, tables)[w].at[me],
            send_sem=a_send.at[w, k],
            recv_sem=a_recv.at[w, k],
            device_id=(target, tp),
            device_id_type=MESH,
        )

    def relay(w, k):
        block = (gathered, tables)[w].at[partner]
        return pltpu.make_async_remote_copy(
            src_ref=block,
            dst_ref=block,
            send_sem=b_send.at[w, k],
            recv_sem=b_recv.at[w, k],
            device_id=(base + (me + k) % side, tp),
            device_id_type=MESH,
        )

    @pl.loop(0, side)
    def _(k):
        for w in range(2):
            spread(w, k).start()

    def mix(target):
        e = target % EXPERTS
        want = (
            lax.broadcasted_iota(jnp.int32, (cap, tok_rows), 0) * copies + target // EXPERTS
        ).astype(F32)
        scale = jnp.where(ranks[pl.ds(e, 1), :] == want, scales[pl.ds(e, 1), :], 0.0)
        where = pl.ds(pl.multiple_of(target * cap, cap), cap)
        high = scale.astype(BF16)
        mix_high[where, :] = high
        mix_low[where, :] = (scale - high.astype(F32)).astype(BF16)

    def fill(source, tok, table):
        want = (
            lax.broadcasted_iota(jnp.int32, (cap, tok_rows), 0) * copies + me // EXPERTS
        ).astype(F32)
        chosen = jnp.where(table == want, 1.0, 0.0).astype(BF16)
        rows[
            pl.ds(pl.multiple_of(source * cap, cap), cap),
            pl.ds(pl.multiple_of(tp * feats, feats), feats),
        ] = jnp.dot(chosen, tok, preferred_element_type=F32).astype(BF16)

    def give(w, k):
        target = (me + k) % n
        e = target % EXPERTS
        return pltpu.make_async_remote_copy(
            src_ref=down_hbm.at[e] if w == 2 else stage.at[w, e],
            dst_ref=weights.at[w, pl.ds(pl.multiple_of(me * depth, depth), depth)],
            send_sem=w_send.at[w, k],
            recv_sem=w_recv.at[w, k],
            device_id=(target, tp),
            device_id_type=MESH,
        )

    for w in range(2):
        for e in range(EXPERTS):
            load(w, e).wait()

        @pl.loop(0, EXPERTS)
        def _(e):
            stage[w, pl.ds(e, 1)] = (
                stage[w, pl.ds(e, 1)].astype(F32) * gain[...][None]
            ).astype(BF16)

        ahead = 1 if w == 0 else 0

        @pl.loop(0, ahead)
        def _(i):
            give(w, shift_of(i, n)).start()

        if w == 0:
            for v in range(2):
                spread(v, 0).wait()

            @pl.loop(1, side)
            def _(k):
                for v in range(2):
                    relay(v, k).start()

        @pl.loop(ahead, n - 1)
        def _(i):
            give(w, shift_of(i, n)).start()

        weights[w, pl.ds(pl.multiple_of(me * depth, depth), depth), :] = stage[
            w, pl.ds(me % EXPERTS, 1)
        ][0]

    @pl.loop(0, n - 1)
    def _(i):
        give(2, shift_of(n - 2 - i, n)).start()

    def share(k):
        block = rows.at[:, pl.ds(pl.multiple_of(tp * feats, feats), feats)]
        return pltpu.make_async_remote_copy(
            src_ref=block,
            dst_ref=block,
            send_sem=f_send.at[k],
            recv_sem=f_recv.at[k],
            device_id=(me, (tp + k) % m),
            device_id_type=MESH,
        )

    @pl.loop(1, side)
    def _(k):
        for w in range(2):
            spread(w, k).wait()
            relay(w, k).wait()

    expert = pl.ds(me % EXPERTS, 1)

    @pl.loop(1, n)
    def _(k):
        source = (me + k) % n
        fill(source, gathered[source], tables[source, expert, :])

    fill(me, tokens[...], ranks[expert, :])

    @pl.loop(1, m)
    def _(k):
        share(k).start()

    @pl.loop(0, n)
    def _(d):
        mix(d)

    @pl.loop(1, m)
    def _(k):
        share(k).wait()

    tile = slots // 12

    @pl.loop(0, slots // tile)
    def _(i):
        where = pl.ds(pl.multiple_of(i * tile, tile), tile)
        value = rows[where, :].astype(F32)
        inverse = lax.rsqrt(jnp.mean(value * value, axis=1, keepdims=True) + EPSILON)
        rows[where, :] = (value * inverse).astype(BF16)

    outs = []
    for w in range(2):

        @pl.loop(1, n)
        def _(k):
            give(w, k).wait()

        outs.append(
            pltpu.make_async_copy(weights.at[w], (gate_out, up_out)[w].at[0], o_sem.at[w])
        )
        outs[w].start()

    big = slots // 6

    @pl.loop(0, slots // big)
    def _(i):
        where = pl.ds(pl.multiple_of(i * big, big), big)
        value = rows[where, :]
        gate_val = jnp.dot(value, weights[0], preferred_element_type=F32)
        up_val = jnp.dot(value, weights[1], preferred_element_type=F32)
        active[where, :] = (gate_val / (1.0 + jnp.exp(-gate_val)) * up_val).astype(BF16)

    def source_of(i):
        k = jnp.where(i == 0, 0, shift_of(n - 2 - jnp.maximum(i - 1, 0), n))
        return k, (me + n - k) % n

    def hand(j):
        owner = j // per
        k = (owner + m - tp) % m
        return pltpu.make_async_remote_copy(
            src_ref=parts.at[j],
            dst_ref=landed.at[j % per, k],
            send_sem=p_send.at[j],
            recv_sem=p_recv.at[j % per, k],
            device_id=(me, owner),
            device_id_type=MESH,
        )

    def taken(q, k):
        return pltpu.make_async_remote_copy(
            src_ref=parts.at[0],
            dst_ref=landed.at[q, k],
            send_sem=p_send.at[0],
            recv_sem=p_recv.at[q, k],
            device_id=(me, (tp + k) % m),
            device_id_type=MESH,
        )

    def back(q, k):
        target = (me + k) % n
        return pltpu.make_async_remote_copy(
            src_ref=result.at[q, pl.ds(pl.multiple_of(target * cap, cap), cap)],
            dst_ref=returned.at[q, pl.ds(pl.multiple_of(me * cap, cap), cap)],
            send_sem=r_send.at[q, k],
            recv_sem=r_recv.at[q, k],
            device_id=(target, tp),
            device_id_type=MESH,
        )

    own_down.wait()
    half = slots // 4

    @pl.loop(0, n + 1)
    def _(i):
        @pl.when(i < n)
        def _():
            k, j = source_of(i)

            @pl.when(i > 0)
            def _():
                give(2, k).wait()

            rhs = weights[2, pl.ds(pl.multiple_of(j * depth, depth), depth), :]

            @pl.loop(0, slots // half)
            def _(r):
                where = pl.ds(pl.multiple_of(r * half, half), half)
                parts[j, where, :] = lax.dot_general(
                    active[where, :], rhs, NT, preferred_element_type=F32
                ).astype(BF16)

            @pl.when(j // per != tp)
            def _():
                hand(j).start()

        @pl.when(i > 0)
        def _():
            _, j = source_of(jnp.maximum(i - 1, 0))
            q = j % per

            @pl.when(j // per == tp)
            def _():
                @pl.loop(1, m)
                def _(k):
                    taken(q, k).wait_recv()

                @pl.loop(0, slots // half)
                def _(r):
                    where = pl.ds(pl.multiple_of(r * half, half), half)
                    total = parts[j, where, :].astype(F32)
                    for k in range(1, m):
                        total = total + landed[q, k, where, :].astype(F32)
                    result[q, where, :] = total.astype(BF16)

                @pl.loop(0, n - 1)
                def _(s):
                    back(q, shift_of(s, n)).start()

                mine = pl.ds(pl.multiple_of(me * cap, cap), cap)
                returned[q, mine, :] = result[q, mine, :]

    last = pltpu.make_async_copy(weights.at[2], down_out.at[0], o_sem.at[2])
    last.start()

    @pl.loop(0, n)
    def _(j):
        @pl.when(j // per != tp)
        def _():
            hand(j).wait_send()

    for q in range(per):

        @pl.loop(1, n)
        def _(k):
            back(q, k).wait()

        value = returned[q]
        total = lax.dot_general(mix_high[...], value, TN, preferred_element_type=F32)
        total += lax.dot_general(mix_low[...], value, TN, preferred_element_type=F32)
        mixed[:, q * depth : (q + 1) * depth] = total.astype(BF16)

    for out in outs:
        out.wait()
    last.wait()


def shards(n, m, tokens, norm_gain, gate_train, up_train, down_train, routes, route_logits):
    experts, depth, width = gate_train.shape
    tok_rows, feats = tokens.shape
    copies = n // experts
    cap = tok_rows // 2 // copies
    slots = n * cap
    per = n // m
    full = jax.ShapeDtypeStruct((1, depth * n, width), BF16)
    vmem = pl.BlockSpec(memory_space=pltpu.VMEM)
    hbm = pl.BlockSpec(memory_space=pl.ANY)
    dma = pltpu.SemaphoreType.DMA
    return pl.pallas_call(
        functools.partial(kernel, n, m),
        out_shape=(full, full, full, jax.ShapeDtypeStruct((tok_rows, feats), BF16)),
        in_specs=[vmem, vmem, hbm, hbm, hbm, vmem, vmem],
        out_specs=(hbm, hbm, hbm, vmem),
        scratch_shapes=[
            pltpu.VMEM((2, experts, depth, width), BF16),
            pltpu.VMEM((3, depth * n, width), BF16),
            pltpu.VMEM((n, tok_rows, feats), BF16),
            pltpu.VMEM((n, experts, tok_rows), F32),
            pltpu.VMEM((slots, feats * m), BF16),
            pltpu.VMEM((slots, width), BF16),
            pltpu.VMEM((experts, tok_rows), F32),
            pltpu.VMEM((experts, tok_rows), F32),
            pltpu.VMEM((slots, tok_rows), BF16),
            pltpu.VMEM((slots, tok_rows), BF16),
            pltpu.VMEM((n, slots, depth), BF16),
            pltpu.VMEM((per, m, slots, depth), BF16),
            pltpu.VMEM((per, slots, depth), BF16),
            pltpu.VMEM((per, slots, depth), BF16),
            dma((3, experts)),
            dma((3, n)),
            dma((3, n)),
            dma((2, n // 2)),
            dma((2, n // 2)),
            dma((2, n // 2)),
            dma((2, n // 2)),
            dma((m,)),
            dma((m,)),
            dma((n,)),
            dma((per, m)),
            dma((per, n)),
            dma((per, n)),
            dma((3,)),
        ],
        compiler_params=pltpu.CompilerParams(
            collective_id=0, has_side_effects=True, vmem_limit_bytes=67043328
        ),
    )(
        tokens,
        norm_gain[:, None],
        gate_train,
        up_train,
        down_train,
        routes.T,
        route_logits.T,
    )


def solution(mesh):
    weight = P(None, "fs", "tp")
    placed = (P("fs", "tp"), P("fs"), weight, weight, weight, P("fs", None), P("fs", None))
    copy = P("fs", None, "tp")
    return jax.shard_map(
        functools.partial(shards, mesh.shape["fs"], mesh.shape["tp"]),
        mesh=mesh,
        in_specs=placed,
        out_specs=(copy, copy, copy, P("fs", "tp")),
        check_vma=False,
    )
```
